32 devices in a mesh: gr: 2 (over x), fs: 8 (over z, y), tp: 2 (over core).
Axes of the slice: x: 2, y: 2, z: 4, core: 2. Of those that a mesh axis runs over, the one named last changes fastest.
Arguments:
- tokens: bfloat16 [4096, 2048], P(('gr', 'fs', 'tp')), may hold values from -6 to 6
- routes: int32 [4096, 8], P(('gr', 'fs', 'tp')), may hold values from 0 to 15, all different within a row; in each aligned block of 128 rows (0 to 127, 128 to 255, ...) at most 96 rows name the same one
- route_weights: float32 [4096, 8], P(('gr', 'fs', 'tp')), may hold values from 0.1 to 0.6
- norm_gain: float32 [2048], P(('gr', 'tp')), may hold values from 0.1 to 1.9
- gate_trained: float32 [16, 384, 2048], P(None, 'fs', ('gr', 'tp')), may hold values from -0.125 to 0.125
- up_trained: float32 [16, 384, 2048], P(None, 'fs', ('gr', 'tp')), may hold values from -0.125 to 0.125
- down_trained: float32 [16, 384, 2048], P(None, 'fs', ('gr', 'tp')), may hold values from -0.3125 to 0.3125
- shared_gate_trained: float32 [512, 2048], P('fs', ('gr', 'tp')), may hold values from -0.125 to 0.125
- shared_up_trained: float32 [512, 2048], P('fs', ('gr', 'tp')), may hold values from -0.125 to 0.125
- shared_down_trained: float32 [512, 2048], P('fs', ('gr', 'tp')), may hold values from -0.25 to 0.25
Outputs:
- combined: bfloat16 [4096, 2048], P(('gr', 'fs', 'tp'))
- expert_gate: bfloat16 [16, 384, 2048], P(('fs', 'tp'))
- expert_up: bfloat16 [16, 384, 2048], P(('fs', 'tp'))
- expert_down: bfloat16 [16, 384, 2048], P(('fs', 'tp'))
- shared_gate: bfloat16 [512, 2048], P('fs')
- shared_up: bfloat16 [512, 2048], P('fs')
- shared_down: bfloat16 [512, 2048], P('fs')
The draws below stay inside these ranges and needn't reach their ends.
Inputs may be any that keep to these rules, and one draw needn't show every extreme that they name: `routes`: each row names 8 different experts. Among the rows of one device no expert is named more than 96 times, and that many is reached in every draw.
All inputs are finite; a program needn't handle non-finite values.
Results may differ from the reference program's by a relative error of at most 0.0084.
Values may be sent and summed in bfloat16 or wider, within the bound.
A program may use at most 128 MiB of HBM per device.

```python
import math
import jax
import jax.numpy as jnp
import numpy as np
from jax import lax

D = 2048
HE = 384
SH = 512
TOP_K = 8
TOK_DEV = 128
EXPERTS = 16
CAP = 96
TOKENS = 4096
N_GR = 2
N_FS = 8
N_TP = 2


def block_levels(rng, extent, split, smallest, largest):
    def one(axis_at, shards_of):
        steps = jax.random.uniform(jax.random.fold_in(jax.random.fold_in(rng, 6), axis_at), (shards_of,), jnp.float32, smallest / len(split), largest / len(split))
        return jnp.repeat(jnp.exp(steps), extent[axis_at] // shards_of).reshape((-1,) + (1,) * (len(extent) - axis_at - 1))

    factor_of = one(*split[0])
    for cut in split[1:]:
        factor_of = factor_of * one(*cut)
    return factor_of


def routed_block(key, own, number, rows, count, top, bound, lean):
    sequence = jax.random.permutation(key, count)
    crowded, common = shares(count, rows * top, bound, lean, True), shares(count, rows * top, bound, lean, False)
    places = jnp.arange(count)

    def named(tallies, turn):
        used = int((tallies > 0).sum())
        fixed = max(1, used // 4)
        passed = fixed + (places - fixed + turn * (used - fixed)) % max(1, count - fixed)
        return jnp.zeros((count,), jnp.int32).at[sequence[jnp.where(places < fixed, places, passed)]].set(jnp.asarray(tallies, jnp.int32))

    tallies = jnp.where(number % 4 == 0, named(crowded, number // 4), named(common, number - number // 4 - 1))
    mixed = jax.random.permutation(jax.random.fold_in(own, 3), count)
    source_of, receiver = mixed[0:count // 2 * 2:2], mixed[1:count // 2 * 2:2]
    margin = jnp.minimum(tallies[source_of] - 1, bound - tallies[receiver]) // 2
    margin = jnp.where((source_of == sequence[0]) | (receiver == sequence[0]) | (tallies[receiver] == 0), 0, jnp.maximum(margin, 0))
    passed = jax.random.randint(jax.random.fold_in(own, 4), (count // 2,), 0, 1 << 20) % (margin + 1)
    tallies = tallies.at[source_of].add(-passed).at[receiver].add(passed)
    members = jnp.searchsorted(jnp.cumsum(tallies), jnp.arange(rows * top), side="right").astype(jnp.int32)
    table = members.reshape(top, rows).T
    table = table[jax.random.permutation(jax.random.fold_in(own, 1), rows)]
    turn = jax.random.randint(jax.random.fold_in(own, 2), (rows, 1), 0, top)
    return jnp.take_along_axis(table, (jnp.arange(top)[None, :] + turn) % top, axis=1)


def shares(amount, total, most, lean, full):
    weights = [(1 << 20) // math.isqrt(rank ** lean) + 1 for rank in range(1, amount + 1)]
    largest = most if full else min(most, max(-(-total // amount), total * weights[0] // sum(weights)))
    least = 1 if total - largest >= amount - 1 else 0
    holding, rest = [largest] + [least] * (amount - 1), total - largest - least * (amount - 1)
    while rest > 0:
        candidates = [i for i in range(1, amount) if holding[i] < largest] or [i for i in range(1, amount) if holding[i] < most]
        pool, remaining = sum([weights[i] for i in candidates]), rest
        for i in candidates:
            more = min(most - holding[i], max(1, remaining * weights[i] // pool), rest)
            holding[i] = holding[i] + more
            rest = rest - more
    return np.array(holding)


def scatter_about(own_key, extent, scale, most, pieces=(), kind=jnp.bfloat16):
    drawn = jax.random.normal(own_key, extent, jnp.float32) * scale
    if len(pieces) > 0:
        drawn = block_levels(own_key, extent, pieces, -0.22, 0.18) * drawn
    return jnp.clip(drawn, min=-most, max=most).astype(kind)


def setup_inputs(seed: int = 0) -> dict:
    key_of = jax.random.split(jax.random.key(seed), 11)
    tokens = scatter_about(key_of[0], (TOKENS, D), 1.0, 6.0, ((0, 32),))
    routes_keys = jax.random.split(jax.random.fold_in(key_of[1], 1), TOKENS // TOK_DEV)
    routes_turns = jax.random.permutation(jax.random.fold_in(key_of[1], 3), TOKENS // TOK_DEV)
    routes = jax.vmap(lambda own, number: routed_block(jax.random.fold_in(key_of[1], 2), own, number, TOK_DEV, EXPERTS, TOP_K, CAP, 1))(routes_keys, routes_turns).reshape((TOKENS, TOP_K))
    route_weights = jnp.clip(0.1 + 0.5 * jax.random.uniform(key_of[2], (TOKENS, TOP_K), jnp.float32) ** block_levels(key_of[2], (TOKENS, TOP_K), ((0, 32),), -0.2, 0.2), 0.1, 0.6)
    norm_gain = jnp.clip(1.0 + 0.18 * jax.random.normal(key_of[3], (D,), jnp.float32), 0.1, 1.9)
    gate_trained = scatter_about(key_of[4], (EXPERTS, HE, D), D ** -0.5, 0.125, ((1, 8), (2, 4)), jnp.float32)
    up_trained = scatter_about(key_of[5], (EXPERTS, HE, D), D ** -0.5, 0.125, ((1, 8), (2, 4)), jnp.float32)
    down_trained = scatter_about(key_of[6], (EXPERTS, HE, D), HE ** -0.5, 0.3125, ((1, 8), (2, 4)), jnp.float32)
    shared_gate_trained = scatter_about(key_of[7], (SH, D), D ** -0.5, 0.125, ((0, 8), (1, 4)), jnp.float32)
    shared_up_trained = scatter_about(key_of[8], (SH, D), D ** -0.5, 0.125, ((0, 8), (1, 4)), jnp.float32)
    shared_down_trained = scatter_about(key_of[9], (SH, D), SH ** -0.5, 0.25, ((0, 8), (1, 4)), jnp.float32)
    return dict(tokens=tokens, routes=routes, route_weights=route_weights, norm_gain=norm_gain, gate_trained=gate_trained, up_trained=up_trained, down_trained=down_trained, shared_gate_trained=shared_gate_trained, shared_up_trained=shared_up_trained, shared_down_trained=shared_down_trained)


epsilon = 1e-06

def contract_rows(inputs, matrix):
    return lax.dot_general(inputs, matrix, (((1,), (1,)), ((), ())), preferred_element_type=jnp.float32)

def swiglu_rows(inputs, gate_matrix, up_matrix, down_matrix):
    hidden = (jax.nn.silu(contract_rows(inputs, gate_matrix)) * contract_rows(inputs, up_matrix)).astype(jnp.bfloat16)
    return jnp.dot(hidden, down_matrix, preferred_element_type=jnp.float32)

def reference(tokens, routes, route_weights, norm_gain, gate_trained, up_trained, down_trained, shared_gate_trained, shared_up_trained, shared_down_trained):
    expert_gate = (gate_trained * norm_gain[None, None, :]).astype(jnp.bfloat16)
    expert_up = (up_trained * norm_gain[None, None, :]).astype(jnp.bfloat16)
    expert_down = down_trained.astype(jnp.bfloat16)
    shared_gate = (shared_gate_trained * norm_gain[None, :]).astype(jnp.bfloat16)
    shared_up = (shared_up_trained * norm_gain[None, :]).astype(jnp.bfloat16)
    shared_down = shared_down_trained.astype(jnp.bfloat16)
    values = tokens.astype(jnp.float32)
    normed = (values * lax.rsqrt(lax.optimization_barrier(jnp.mean(values * values, axis=1, keepdims=True)) + epsilon)).astype(jnp.bfloat16)
    shared_out = swiglu_rows(normed, shared_gate, shared_up, shared_down)
    chosen = routes.reshape(-1).astype(jnp.int32)
    order = jnp.argsort(chosen, stable=True).astype(jnp.int32)
    sorted_tokens = (order // TOP_K).astype(jnp.int32)
    sorted_weights = route_weights.reshape(-1)[order]
    counts = jnp.bincount(chosen, length=EXPERTS).astype(jnp.int32)
    firsts = (jnp.cumsum(counts) - counts).astype(jnp.int32)
    limit = N_GR * N_FS * N_TP * CAP
    last_place = chosen.shape[0] - 1

    def per_expert(running, expert):
        offsets = jnp.arange(limit, dtype=jnp.int32)
        places = jnp.minimum(firsts[expert] + offsets, last_place).astype(jnp.int32)
        valid = offsets < counts[expert]
        rows_in = sorted_tokens[places]
        weights = jnp.where(valid, sorted_weights[places], jnp.zeros_like(sorted_weights[places]))
        result = swiglu_rows(normed[rows_in], expert_gate[expert], expert_up[expert], expert_down[expert]).astype(jnp.bfloat16)
        return (running.at[rows_in].add(weights[:, None] * result.astype(jnp.float32)), None)
    routed, _ = lax.scan(per_expert, jnp.zeros(tokens.shape, jnp.float32), jnp.arange(EXPERTS, dtype=jnp.int32))
    combined = (routed + shared_out).astype(jnp.bfloat16)
    return (combined, expert_gate, expert_up, expert_down, shared_gate, shared_up, shared_down)
```

```python
import functools

import jax
import jax.numpy as jnp
from jax import lax
from jax.experimental import pallas as pl
from jax.experimental.pallas import tpu as pltpu
from jax.sharding import PartitionSpec as P

epsilon = 1e-06
LANES = 128
MESH = pl.DeviceIdType.MESH


def contract_rows(inputs, matrix):
    return lax.dot_general(
        inputs, matrix, (((1,), (1,)), ((), ())), preferred_element_type=jnp.float32
    )


def swiglu_rows(inputs, gate_matrix, up_matrix, down_matrix):
    hidden = (
        jax.nn.silu(contract_rows(inputs, gate_matrix)) * contract_rows(inputs, up_matrix)
    ).astype(jnp.bfloat16)
    return jnp.dot(hidden, down_matrix, preferred_element_type=jnp.float32)


def dispatch_body(
    tokens,
    routes,
    route_weights,
    norm_gain,
    gate_trained,
    up_trained,
    down_trained,
    shared_gate_trained,
    shared_up_trained,
    shared_down_trained,
):
    gain_row = norm_gain[None, None, :]
    stacked = jnp.stack(
        [gate_trained * gain_row, up_trained * gain_row, down_trained], axis=1
    ).astype(jnp.bfloat16)
    halves = lax.all_to_all(
        lax.all_to_all(stacked[:, :, :, None, :], "fs", split_axis=0, concat_axis=2, tiled=True),
        "tp",
        split_axis=0,
        concat_axis=3,
        tiled=True,
    )
    owned = lax.all_gather(halves[:, :, :, None], "gr", axis=3, tiled=True)
    owned = owned.reshape(owned.shape[0], 3, owned.shape[2], -1)
    expert_gate = owned[:, 0]
    expert_up = owned[:, 1]
    expert_down = owned[:, 2]
    shared_gain = norm_gain[None, :]
    shared_stack = jnp.stack(
        [shared_gate_trained * shared_gain, shared_up_trained * shared_gain, shared_down_trained],
        axis=0,
    ).astype(jnp.bfloat16)
    shared_whole = lax.all_gather(shared_stack, ("gr", "tp"), axis=2, tiled=True)
    shared_gate = shared_whole[0]
    shared_up = shared_whole[1]
    shared_down = shared_whole[2]
    values = tokens.astype(jnp.float32)
    normed = (
        values * lax.rsqrt(jnp.mean(values * values, axis=1, keepdims=True) + epsilon)
    ).astype(jnp.bfloat16)
    row_count, features = normed.shape
    per_token = routes.shape[1]
    shared_out = swiglu_rows(
        normed,
        lax.all_gather(shared_gate, "fs", axis=0, tiled=True),
        lax.all_gather(shared_up, "fs", axis=0, tiled=True),
        lax.all_gather(shared_down, "fs", axis=0, tiled=True),
    )
    experts = lax.axis_size("fs") * lax.axis_size("tp")
    capacity = max(2, 3 * row_count * per_token // (2 * experts))
    chosen = routes.reshape(-1)
    onehot = (chosen[:, None] == jnp.arange(experts, dtype=jnp.int32)[None, :]).astype(jnp.int32)
    position = jnp.sum((jnp.cumsum(onehot, axis=0) - onehot) * onehot, axis=1)
    target = chosen * capacity + position
    source = (
        jnp.full((experts * capacity,), row_count, jnp.int32)
        .at[target]
        .set(jnp.arange(row_count * per_token, dtype=jnp.int32) // per_token)
    )
    padded = jnp.concatenate([normed, jnp.zeros((1, features), jnp.bfloat16)], axis=0)
    outgoing = padded[source].reshape(experts, capacity, features)
    arrived = lax.all_to_all(outgoing, ("fs", "tp"), split_axis=0, concat_axis=0, tiled=True)
    item_count = arrived.shape[1]
    result = swiglu_rows(
        arrived.reshape(-1, features), expert_gate[0], expert_up[0], expert_down[0]
    )
    result = result.astype(jnp.bfloat16).reshape(experts, item_count, features)
    returned = lax.all_to_all(result, ("fs", "tp"), split_axis=0, concat_axis=0, tiled=True)
    picked = returned.reshape(experts * capacity, features)[target].astype(jnp.float32)
    picked = picked.reshape(row_count, per_token, features)
    routed = jnp.sum(picked * route_weights[:, :, None], axis=1)
    combined = (routed + shared_out).astype(jnp.bfloat16)
    return (combined, expert_gate, expert_up, expert_down, shared_gate, shared_up, shared_down)


def exchange_kernel(
    n,
    pieces_ref,
    shared_ref,
    rows_ref,
    combined_ref,
    gate_ref,
    up_ref,
    down_ref,
    shared_gate_ref,
    shared_up_ref,
    shared_down_ref,
    weights,
    shared,
    rows,
    parts,
    pair_in,
    sums,
    sums_in,
    local_sem,
    piece_sem,
    weight_sem,
    column_out_sem,
    column_sem,
    shared_out_sem,
    shared_sem,
    row_out_sem,
    row_sem,
    row_pair_out_sem,
    row_pair_sem,
    part_sem,
    part_recv_sem,
    sum_sem,
    sum_recv_sem,
    out_sem,
):
    gr, fs, tp = lax.axis_index("gr"), lax.axis_index("fs"), lax.axis_index("tp")
    other = 1 - tp
    across = (1 - gr, fs, tp)
    twin = (gr, fs, other)
    expert = fs * 2 + tp
    hidden_piece, width = pieces_ref.shape[2], pieces_ref.shape[3]
    hidden = n * hidden_piece
    shared_piece = shared_ref.shape[1]
    extra = shared_piece // 2
    features = 4 * width
    row_count = rows_ref.shape[0]

    barrier = pltpu.get_barrier_semaphore()
    pl.semaphore_signal(barrier, inc=1, device_id=across, device_id_type=MESH)
    pl.semaphore_signal(barrier, inc=1, device_id=twin, device_id_type=MESH)
    for k in range(1, n):
        for t in range(2):
            pl.semaphore_signal(
                barrier, inc=1, device_id=(gr, lax.rem(fs + k, n), t), device_id_type=MESH
            )
    pl.semaphore_wait(barrier, 2 * n)

    def remote(src, dst, send, recv, device):
        return pltpu.make_async_remote_copy(
            src_ref=src,
            dst_ref=dst,
            send_sem=send,
            recv_sem=recv,
            device_id=device,
            device_id_type=MESH,
        )

    def columns(g, t):
        return pl.ds(pl.multiple_of((g * 2 + t) * width, width), width)

    def slab(source, span):
        start = pl.multiple_of(source * hidden_piece, 16)
        return weights.at[:, pl.ds(start, hidden_piece), span]

    def row_block(source, t):
        start = pl.multiple_of((source * 2 + t) * row_count, row_count)
        return rows.at[pl.ds(start, row_count)]

    half = pl.ds(pl.multiple_of(gr * 2 * width, width), 2 * width)
    far_half = pl.ds(pl.multiple_of((1 - gr) * 2 * width, width), 2 * width)

    def piece_send(d, t):
        return remote(
            pieces_ref.at[d * 2 + t],
            slab(fs, columns(gr, tp)),
            piece_sem.at[d, t],
            weight_sem.at[fs, tp],
            (gr, d, t),
        )

    def column_send(source):
        return remote(slab(source, half), slab(source, half), column_out_sem.at[source], column_sem.at[source], across)

    def row_send(d):
        return remote(rows_ref, row_block(fs, tp), row_out_sem.at[d], row_sem.at[fs], (gr, d, tp))

    own_piece = pltpu.make_async_copy(
        pieces_ref.at[expert], slab(fs, columns(gr, tp)), local_sem.at[0]
    )
    own_shared = pltpu.make_async_copy(
        shared_ref, shared.at[:, :, columns(gr, tp)], local_sem.at[1]
    )
    own_rows = pltpu.make_async_copy(rows_ref, row_block(fs, tp), local_sem.at[2])
    own_piece.start()
    own_shared.start()
    own_rows.start()

    twin_piece = piece_send(fs, other)
    twin_piece.start()
    shared_far = remote(
        shared_ref, shared.at[:, :, columns(gr, tp)], shared_out_sem.at[0], shared_sem.at[0], across
    )
    shared_far.start()
    shared_twin = remote(
        shared_ref, shared.at[:, :, columns(gr, tp)], shared_out_sem.at[1], shared_sem.at[1], twin
    )
    shared_twin.start()

    for k in range(1, n):
        d = lax.rem(fs + k, n)
        piece_send(d, 0).start()
        piece_send(d, 1).start()
    for k in range(1, n):
        row_send(lax.rem(fs + n - k, n)).start()
    row_twin = remote(rows_ref, row_block(fs, tp), row_pair_out_sem.at[fs], row_pair_sem.at[fs], twin)
    row_twin.start()

    own_piece.wait()
    twin_arrival = remote(
        pieces_ref.at[0], slab(fs, columns(gr, other)), piece_sem.at[fs, other], weight_sem.at[fs, other], twin
    )
    twin_arrival.wait_recv()
    column_send(fs).start()

    for k in range(1, n):
        source = lax.rem(fs + n - k, n)
        for t in range(2):
            remote(
                pieces_ref.at[0],
                slab(source, columns(gr, t)),
                piece_sem.at[fs, other],
                weight_sem.at[source, t],
                twin,
            ).wait_recv()
        column_send(source).start()

    own_shared.wait()
    far_columns = shared.at[:, :, columns(1 - gr, tp)]
    remote(shared_ref, far_columns, shared_out_sem.at[0], shared_sem.at[0], across).wait_recv()
    shared_relay = remote(far_columns, far_columns, shared_out_sem.at[2], shared_sem.at[2], twin)
    shared_relay.start()
    remote(
        shared_ref, shared.at[:, :, columns(gr, other)], shared_out_sem.at[1], shared_sem.at[1], twin
    ).wait_recv()
    last_columns = shared.at[:, :, columns(1 - gr, other)]
    remote(shared_ref, last_columns, shared_out_sem.at[2], shared_sem.at[2], twin).wait_recv()
    tail = pltpu.make_async_copy(
        shared.at[:, pl.ds(pl.multiple_of(tp * extra, extra), extra), :],
        weights.at[:, pl.ds(hidden, extra), :],
        local_sem.at[3],
    )
    tail.start()

    own_rows.wait()

    def row_relay(source):
        return remote(
            row_block(source, tp),
            row_block(source, tp),
            row_pair_out_sem.at[source],
            row_pair_sem.at[source],
            twin,
        )

    for k in range(1, n):
        source = lax.rem(fs + k, n)
        remote(rows_ref, row_block(source, tp), row_out_sem.at[source], row_sem.at[source], twin).wait_recv()
        row_relay(source).start()

    for k in range(n):
        source = lax.rem(fs + n - k, n)
        remote(
            slab(source, far_half),
            slab(source, far_half),
            column_out_sem.at[source],
            column_sem.at[source],
            across,
        ).wait_recv()
    tail.wait()
    outs = []
    for j, ref in enumerate((gate_ref, up_ref, down_ref)):
        outs.append(
            pltpu.make_async_copy(weights.at[j, pl.ds(0, hidden), :], ref.at[0], out_sem.at[j])
        )
    for j, ref in enumerate((shared_gate_ref, shared_up_ref, shared_down_ref)):
        outs.append(pltpu.make_async_copy(shared.at[j], ref, out_sem.at[3 + j]))
    for copy in outs:
        copy.start()

    def part_send(k):
        return pltpu.make_async_remote_copy(
            src_ref=parts.at[k, pl.ds(pl.multiple_of(other * row_count, row_count), row_count), :],
            dst_ref=pair_in.at[k],
            send_sem=part_sem.at[k],
            recv_sem=part_recv_sem.at[k],
            device_id=twin,
            device_id_type=MESH,
        )

    def sum_send(k):
        return pltpu.make_async_remote_copy(
            src_ref=sums.at[k],
            dst_ref=sums_in.at[k],
            send_sem=sum_sem.at[k],
            recv_sem=sum_recv_sem.at[k],
            device_id=(gr, lax.rem(fs + 1 + k, n), tp),
            device_id_type=MESH,
        )

    chunk = 32

    def finish(k):
        part_send(k).wait_recv()

        @pl.loop(0, row_count // chunk)
        def _(i):
            at = pl.multiple_of(i * chunk, chunk)
            mine = pl.multiple_of(tp * row_count + i * chunk, chunk)
            value = parts[k, pl.ds(mine, chunk), :].astype(jnp.float32)
            value = value + pair_in[k, pl.ds(at, chunk), :].astype(jnp.float32)
            sums[k, pl.ds(at, chunk), :] = value.astype(jnp.bfloat16)

    @pl.loop(0, n)
    def _(k):
        d = lax.rem(fs + 1 + k, n)
        remote(
            rows_ref, row_block(d, other), row_pair_out_sem.at[d], row_pair_sem.at[d], twin
        ).wait_recv()
        block = pl.ds(pl.multiple_of(d * 2 * row_count, 2 * row_count), 2 * row_count)
        inputs = rows[block, 0:features]
        factors = rows[block, features : features + LANES].astype(jnp.float32)
        lane = lax.broadcasted_iota(jnp.int32, factors.shape, 1)
        chosen = (lane == expert) | (lane == expert + LANES // 2)
        factor = jnp.sum(jnp.where(chosen, factors, 0.0), axis=1, keepdims=True)
        gate = contract_rows(inputs, weights[0])
        up = contract_rows(inputs, weights[1])
        unit = lax.broadcasted_iota(jnp.int32, gate.shape, 1)
        scale = jnp.where(unit < hidden, factor, 1.0)
        units = (gate / (1.0 + jnp.exp(-gate)) * up * scale).astype(jnp.bfloat16)
        for c in range(4):
            span = pl.ds(c * width, width)
            parts[k, :, span] = jnp.dot(
                units, weights[2, :, span], preferred_element_type=jnp.float32
            ).astype(jnp.bfloat16)
        part_send(k).start()

        @pl.when(k > 0)
        def _():
            finish(k - 1)
            sum_send(k - 1).start()

    finish(n - 1)
    for k in range(n - 1):
        sum_send(k).wait_recv()

    @pl.loop(0, row_count // chunk)
    def _(i):
        at = pl.ds(pl.multiple_of(i * chunk, chunk), chunk)
        total = sums[n - 1, at, :].astype(jnp.float32)
        for k in range(n - 1):
            total = total + sums_in[k, at, :].astype(jnp.float32)
        combined_ref[at, :] = total.astype(jnp.bfloat16)

    twin_piece.wait_send()
    shared_far.wait_send()
    shared_twin.wait_send()
    shared_relay.wait_send()
    row_twin.wait_send()
    column_send(fs).wait_send()
    for k in range(1, n):
        piece_send(lax.rem(fs + k, n), 0).wait_send()
        piece_send(lax.rem(fs + k, n), 1).wait_send()
        row_send(lax.rem(fs + k, n)).wait_send()
        column_send(lax.rem(fs + k, n)).wait_send()
        row_relay(lax.rem(fs + k, n)).wait_send()
    for k in range(n):
        part_send(k).wait_send()
    for k in range(n - 1):
        sum_send(k).wait_send()
    for copy in outs:
        copy.wait()


def direct_body(
    tokens,
    routes,
    route_weights,
    norm_gain,
    gate_trained,
    up_trained,
    down_trained,
    shared_gate_trained,
    shared_up_trained,
    shared_down_trained,
):
    gain_row = norm_gain[None, None, :]
    pieces = jnp.stack(
        [gate_trained * gain_row, up_trained * gain_row, down_trained], axis=1
    ).astype(jnp.bfloat16)
    shared_gain = norm_gain[None, :]
    shared_stack = jnp.stack(
        [shared_gate_trained * shared_gain, shared_up_trained * shared_gain, shared_down_trained],
        axis=0,
    ).astype(jnp.bfloat16)
    values = tokens.astype(jnp.float32)
    normed = (
        values * lax.rsqrt(jnp.mean(values * values, axis=1, keepdims=True) + epsilon)
    ).astype(jnp.bfloat16)
    n = lax.axis_size("fs")
    experts, _, hidden_piece, width = pieces.shape
    row_count, features = normed.shape
    shared_piece = shared_stack.shape[1]
    numbers = jnp.arange(LANES // 2, dtype=jnp.int32)
    factors = jnp.sum(
        jnp.where(routes[:, :, None] == numbers, route_weights[:, :, None], 0.0), axis=1
    )
    high = lax.reduce_precision(factors, 8, 7)
    rows = jnp.concatenate(
        [normed, high.astype(jnp.bfloat16), (factors - high).astype(jnp.bfloat16)], axis=1
    )
    hidden = n * hidden_piece
    hidden_all = hidden + shared_piece // 2
    vmem = pl.BlockSpec(memory_space=pltpu.VMEM)
    hbm = pl.BlockSpec(memory_space=pl.ANY)
    kind = jnp.bfloat16
    expert_shape = jax.ShapeDtypeStruct((1, hidden, features), kind)
    shared_shape = jax.ShapeDtypeStruct((shared_piece, features), kind)
    DMA = pltpu.SemaphoreType.DMA
    return pl.pallas_call(
        functools.partial(exchange_kernel, n),
        out_shape=(jax.ShapeDtypeStruct((row_count, features), kind),)
        + (expert_shape,) * 3
        + (shared_shape,) * 3,
        in_specs=[vmem] * 3,
        out_specs=(vmem,) + (hbm,) * 6,
        scratch_shapes=[
            pltpu.VMEM((3, hidden_all, features), kind),
            pltpu.VMEM((3, shared_piece, features), kind),
            pltpu.VMEM((experts * row_count, features + LANES), kind),
            pltpu.VMEM((n, 2 * row_count, features), kind),
            pltpu.VMEM((n, row_count, features), kind),
            pltpu.VMEM((n, row_count, features), kind),
            pltpu.VMEM((n - 1, row_count, features), kind),
            DMA((4,)),
            DMA((n, 2)),
            DMA((n, 2)),
            DMA((n,)),
            DMA((n,)),
            DMA((3,)),
            DMA((3,)),
            DMA((n,)),
            DMA((n,)),
            DMA((n,)),
            DMA((n,)),
            DMA((n,)),
            DMA((n,)),
            DMA((n - 1,)),
            DMA((n - 1,)),
            DMA((6,)),
        ],
        compiler_params=pltpu.CompilerParams(
            collective_id=0, has_side_effects=True, vmem_limit_bytes=60 * 1024 * 1024
        ),
    )(pieces, shared_stack, rows)


def body(*arguments):
    experts = lax.axis_size("fs") * lax.axis_size("tp")
    per_token = arguments[1].shape[1]
    pairs = lax.axis_size("gr") == 2 and lax.axis_size("tp") == 2
    if pairs and experts <= min(2 * per_token, LANES // 2):
        return direct_body(*arguments)
    return dispatch_body(*arguments)


def solution(mesh):
    in_specs = (
        P(("gr", "fs", "tp"), None),
        P(("gr", "fs", "tp"), None),
        P(("gr", "fs", "tp"), None),
        P(("gr", "tp")),
        P(None, "fs", ("gr", "tp")),
        P(None, "fs", ("gr", "tp")),
        P(None, "fs", ("gr", "tp")),
        P("fs", ("gr", "tp")),
        P("fs", ("gr", "tp")),
        P("fs", ("gr", "tp")),
    )
    out_specs = (
        P(("gr", "fs", "tp"), None),
        P(("fs", "tp"), None, None),
        P(("fs", "tp"), None, None),
        P(("fs", "tp"), None, None),
        P("fs", None),
        P("fs", None),
        P("fs", None),
    )
    return jax.shard_map(body, mesh=mesh, in_specs=in_specs, out_specs=out_specs, check_vma=False)
```

```python
import functools

import jax
import jax.numpy as jnp
from jax import lax
from jax.experimental import pallas as pl
from jax.experimental.pallas import tpu as pltpu
from jax.sharding import PartitionSpec as P

epsilon = 1e-06
LANES = 128
MESH = pl.DeviceIdType.MESH


def contract_rows(inputs, matrix):
    return lax.dot_general(
        inputs, matrix, (((1,), (1,)), ((), ())), preferred_element_type=jnp.float32
    )


def swiglu_rows(inputs, gate_matrix, up_matrix, down_matrix):
    hidden = (
        jax.nn.silu(contract_rows(inputs, gate_matrix)) * contract_rows(inputs, up_matrix)
    ).astype(jnp.bfloat16)
    return jnp.dot(hidden, down_matrix, preferred_element_type=jnp.float32)


def dispatch_body(
    tokens,
    routes,
    route_weights,
    norm_gain,
    gate_trained,
    up_trained,
    down_trained,
    shared_gate_trained,
    shared_up_trained,
    shared_down_trained,
):
    gain_row = norm_gain[None, None, :]
    stacked = jnp.stack(
        [gate_trained * gain_row, up_trained * gain_row, down_trained], axis=1
    ).astype(jnp.bfloat16)
    halves = lax.all_to_all(
        lax.all_to_all(stacked[:, :, :, None, :], "fs", split_axis=0, concat_axis=2, tiled=True),
        "tp",
        split_axis=0,
        concat_axis=3,
        tiled=True,
    )
    owned = lax.all_gather(halves[:, :, :, None], "gr", axis=3, tiled=True)
    owned = owned.reshape(owned.shape[0], 3, owned.shape[2], -1)
    expert_gate = owned[:, 0]
    expert_up = owned[:, 1]
    expert_down = owned[:, 2]
    shared_gain = norm_gain[None, :]
    shared_stack = jnp.stack(
        [shared_gate_trained * shared_gain, shared_up_trained * shared_gain, shared_down_trained],
        axis=0,
    ).astype(jnp.bfloat16)
    shared_whole = lax.all_gather(shared_stack, ("gr", "tp"), axis=2, tiled=True)
    shared_gate = shared_whole[0]
    shared_up = shared_whole[1]
    shared_down = shared_whole[2]
    values = tokens.astype(jnp.float32)
    normed = (
        values * lax.rsqrt(jnp.mean(values * values, axis=1, keepdims=True) + epsilon)
    ).astype(jnp.bfloat16)
    row_count, features = normed.shape
    per_token = routes.shape[1]
    shared_out = swiglu_rows(
        normed,
        lax.all_gather(shared_gate, "fs", axis=0, tiled=True),
        lax.all_gather(shared_up, "fs", axis=0, tiled=True),
        lax.all_gather(shared_down, "fs", axis=0, tiled=True),
    )
    experts = lax.axis_size("fs") * lax.axis_size("tp")
    capacity = max(2, 3 * row_count * per_token // (2 * experts))
    chosen = routes.reshape(-1)
    onehot = (chosen[:, None] == jnp.arange(experts, dtype=jnp.int32)[None, :]).astype(jnp.int32)
    position = jnp.sum((jnp.cumsum(onehot, axis=0) - onehot) * onehot, axis=1)
    target = chosen * capacity + position
    source = (
        jnp.full((experts * capacity,), row_count, jnp.int32)
        .at[target]
        .set(jnp.arange(row_count * per_token, dtype=jnp.int32) // per_token)
    )
    padded = jnp.concatenate([normed, jnp.zeros((1, features), jnp.bfloat16)], axis=0)
    outgoing = padded[source].reshape(experts, capacity, features)
    arrived = lax.all_to_all(outgoing, ("fs", "tp"), split_axis=0, concat_axis=0, tiled=True)
    item_count = arrived.shape[1]
    result = swiglu_rows(
        arrived.reshape(-1, features), expert_gate[0], expert_up[0], expert_down[0]
    )
    result = result.astype(jnp.bfloat16).reshape(experts, item_count, features)
    returned = lax.all_to_all(result, ("fs", "tp"), split_axis=0, concat_axis=0, tiled=True)
    picked = returned.reshape(experts * capacity, features)[target].astype(jnp.float32)
    picked = picked.reshape(row_count, per_token, features)
    routed = jnp.sum(picked * route_weights[:, :, None], axis=1)
    combined = (routed + shared_out).astype(jnp.bfloat16)
    return (combined, expert_gate, expert_up, expert_down, shared_gate, shared_up, shared_down)


def exchange_kernel(
    n,
    pieces_ref,
    shared_ref,
    rows_ref,
    combined_ref,
    gate_ref,
    up_ref,
    down_ref,
    shared_gate_ref,
    shared_up_ref,
    shared_down_ref,
    weights,
    shared,
    rows,
    parts,
    pair_in,
    sums,
    side_in,
    sums_in,
    local_sem,
    piece_sem,
    weight_sem,
    column_out_sem,
    column_sem,
    shared_out_sem,
    shared_sem,
    row_out_sem,
    row_side_sem,
    row_back_sem,
    row_sem,
    row_pair_out_sem,
    row_pair_sem,
    part_sem,
    part_recv_sem,
    side_sem,
    side_recv_sem,
    sum_sem,
    sum_recv_sem,
    out_sem,
):
    gr, fs, tp = lax.axis_index("gr"), lax.axis_index("fs"), lax.axis_index("tp")
    other = 1 - tp
    across = (1 - gr, fs, tp)
    twin = (gr, fs, other)
    expert = fs * 2 + tp
    hidden_piece, width = pieces_ref.shape[2], pieces_ref.shape[3]
    hidden = n * hidden_piece
    shared_piece = shared_ref.shape[1]
    extra = shared_piece // 2
    features = 4 * width
    row_count = rows_ref.shape[0]
    depth = n // 2
    outer, inner = lax.div(fs, 2), lax.rem(fs, 2)
    beside = (gr, outer * 2 + 1 - inner, tp)

    barrier = pltpu.get_barrier_semaphore()
    pl.semaphore_signal(barrier, inc=1, device_id=across, device_id_type=MESH)
    pl.semaphore_signal(barrier, inc=1, device_id=twin, device_id_type=MESH)
    for k in range(1, n):
        for t in range(2):
            pl.semaphore_signal(
                barrier, inc=1, device_id=(gr, lax.rem(fs + k, n), t), device_id_type=MESH
            )
    pl.semaphore_wait(barrier, 2 * n)

    def remote(src, dst, send, recv, device):
        return pltpu.make_async_remote_copy(
            src_ref=src,
            dst_ref=dst,
            send_sem=send,
            recv_sem=recv,
            device_id=device,
            device_id_type=MESH,
        )

    def columns(g, t):
        return pl.ds(pl.multiple_of((g * 2 + t) * width, width), width)

    def slab(source, span):
        start = pl.multiple_of(source * hidden_piece, 16)
        return weights.at[:, pl.ds(start, hidden_piece), span]

    def row_block(source, t):
        start = pl.multiple_of((source * 2 + t) * row_count, row_count)
        return rows.at[pl.ds(start, row_count)]

    half = pl.ds(pl.multiple_of(gr * 2 * width, width), 2 * width)
    far_half = pl.ds(pl.multiple_of((1 - gr) * 2 * width, width), 2 * width)

    def piece_send(d, t):
        return remote(
            pieces_ref.at[d * 2 + t],
            slab(fs, columns(gr, tp)),
            piece_sem.at[d, t],
            weight_sem.at[fs, tp],
            (gr, d, t),
        )

    def column_send(source):
        return remote(slab(source, half), slab(source, half), column_out_sem.at[source], column_sem.at[source], across)

    def row_move(source, send, recv, device):
        return remote(row_block(source, tp), row_block(source, tp), send, recv, device)

    def row_onward(source, step):
        return row_move(
            source,
            row_out_sem.at[source],
            row_sem.at[source],
            (gr, (outer + step) * 2 + inner, tp),
        )

    def row_beside(source):
        return row_move(source, row_side_sem.at[lax.div(source, 2)], row_sem.at[source], beside)

    def row_relay(source):
        return row_move(source, row_pair_out_sem.at[source], row_pair_sem.at[source], twin)

    def row_back():
        return row_move(
            fs, row_back_sem.at[0], row_sem.at[fs], (gr, (outer - 1) * 2 + inner, tp)
        )

    def at_distance(action):
        for distance in range(1, depth):
            for step in (1, -1):
                place = outer - step * distance

                @pl.when((place >= 0) & (place < depth))
                def _():
                    action(place, step)

    def onward_exists(step):
        return (outer + step >= 0) & (outer + step < depth)

    own_piece = pltpu.make_async_copy(
        pieces_ref.at[expert], slab(fs, columns(gr, tp)), local_sem.at[0]
    )
    own_shared = pltpu.make_async_copy(
        shared_ref, shared.at[:, :, columns(gr, tp)], local_sem.at[1]
    )
    own_rows = pltpu.make_async_copy(rows_ref, row_block(fs, tp), local_sem.at[2])
    own_rows.start()
    own_piece.start()
    own_shared.start()
    own_rows.wait()

    @pl.when(outer < depth - 1)
    def _():
        row_onward(fs, 1).start()

    @pl.when(outer > 0)
    def _():
        row_back().start()

    row_beside(fs).start()
    row_relay(fs).start()

    twin_piece = piece_send(fs, other)
    twin_piece.start()
    shared_far = remote(
        shared_ref, shared.at[:, :, columns(gr, tp)], shared_out_sem.at[0], shared_sem.at[0], across
    )
    shared_far.start()
    shared_twin = remote(
        shared_ref, shared.at[:, :, columns(gr, tp)], shared_out_sem.at[1], shared_sem.at[1], twin
    )
    shared_twin.start()

    for k in range(1, n):
        d = lax.rem(fs + k, n)
        piece_send(d, 0).start()
        piece_send(d, 1).start()
    own_piece.wait()
    twin_arrival = remote(
        pieces_ref.at[0], slab(fs, columns(gr, other)), piece_sem.at[fs, other], weight_sem.at[fs, other], twin
    )
    twin_arrival.wait_recv()
    column_send(fs).start()

    def take_rows(source):
        row_move(source, row_out_sem.at[source], row_sem.at[source], twin).wait_recv()

    def take_weights(source):
        for t in range(2):
            remote(
                pieces_ref.at[0],
                slab(source, columns(gr, t)),
                piece_sem.at[fs, other],
                weight_sem.at[source, t],
                twin,
            ).wait_recv()
        column_send(source).start()

    def arrive(place, step):
        source = place * 2 + inner
        take_rows(source)

        @pl.when(onward_exists(step))
        def _():
            row_onward(source, step).start()

        row_beside(source).start()
        row_relay(source).start()
        take_weights(source)
        take_weights(place * 2 + 1 - inner)

    def arrive_beside(place, step):
        source = place * 2 + 1 - inner
        take_rows(source)
        row_relay(source).start()

    take_weights(outer * 2 + 1 - inner)
    at_distance(arrive)
    arrive_beside(outer, 0)
    at_distance(arrive_beside)

    own_shared.wait()
    far_columns = shared.at[:, :, columns(1 - gr, tp)]
    remote(shared_ref, far_columns, shared_out_sem.at[0], shared_sem.at[0], across).wait_recv()
    shared_relay = remote(far_columns, far_columns, shared_out_sem.at[2], shared_sem.at[2], twin)
    shared_relay.start()
    remote(
        shared_ref, shared.at[:, :, columns(gr, other)], shared_out_sem.at[1], shared_sem.at[1], twin
    ).wait_recv()
    last_columns = shared.at[:, :, columns(1 - gr, other)]
    remote(shared_ref, last_columns, shared_out_sem.at[2], shared_sem.at[2], twin).wait_recv()
    tail = pltpu.make_async_copy(
        shared.at[:, pl.ds(pl.multiple_of(tp * extra, extra), extra), :],
        weights.at[:, pl.ds(hidden, extra), :],
        local_sem.at[3],
    )
    tail.start()

    for k in range(n):
        source = lax.rem(fs + n - k, n)
        remote(
            slab(source, far_half),
            slab(source, far_half),
            column_out_sem.at[source],
            column_sem.at[source],
            across,
        ).wait_recv()
    tail.wait()
    outs = []
    for j, ref in enumerate((gate_ref, up_ref, down_ref)):
        outs.append(
            pltpu.make_async_copy(weights.at[j, pl.ds(0, hidden), :], ref.at[0], out_sem.at[j])
        )
    for j, ref in enumerate((shared_gate_ref, shared_up_ref, shared_down_ref)):
        outs.append(pltpu.make_async_copy(shared.at[j], ref, out_sem.at[3 + j]))
    for copy in outs:
        copy.start()

    def part_send(k):
        return pltpu.make_async_remote_copy(
            src_ref=parts.at[k, pl.ds(pl.multiple_of(other * row_count, row_count), row_count), :],
            dst_ref=pair_in.at[k],
            send_sem=part_sem.at[k],
            recv_sem=part_recv_sem.at[k],
            device_id=twin,
            device_id_type=MESH,
        )

    def place_of(k):
        return lax.rem(outer + 1 + lax.rem(k, depth), depth)

    def side_send(k):
        return pltpu.make_async_remote_copy(
            src_ref=sums.at[k],
            dst_ref=side_in.at[k],
            send_sem=side_sem.at[k],
            recv_sem=side_recv_sem.at[k],
            device_id=beside,
            device_id_type=MESH,
        )

    def sum_send(k):
        return pltpu.make_async_remote_copy(
            src_ref=sums.at[k],
            dst_ref=sums_in.at[k - depth],
            send_sem=sum_sem.at[k - depth],
            recv_sem=sum_recv_sem.at[k - depth],
            device_id=(gr, place_of(k) * 2 + inner, tp),
            device_id_type=MESH,
        )

    chunk = 32

    def add_pair(k):
        part_send(k).wait_recv()

        @pl.loop(0, row_count // chunk)
        def _(i):
            at = pl.multiple_of(i * chunk, chunk)
            mine = pl.multiple_of(tp * row_count + i * chunk, chunk)
            value = parts[k, pl.ds(mine, chunk), :].astype(jnp.float32)
            value = value + pair_in[k, pl.ds(at, chunk), :].astype(jnp.float32)
            sums[k, pl.ds(at, chunk), :] = value.astype(jnp.bfloat16)

    def add_both(k):
        part_send(k).wait_recv()
        side_send(k - depth).wait_recv()

        @pl.loop(0, row_count // chunk)
        def _(i):
            at = pl.multiple_of(i * chunk, chunk)
            mine = pl.multiple_of(tp * row_count + i * chunk, chunk)
            value = parts[k, pl.ds(mine, chunk), :].astype(jnp.float32)
            value = value + pair_in[k, pl.ds(at, chunk), :].astype(jnp.float32)
            value = value + side_in[k - depth, pl.ds(at, chunk), :].astype(jnp.float32)
            sums[k, pl.ds(at, chunk), :] = value.astype(jnp.bfloat16)

    @pl.loop(0, n)
    def _(k):
        d = place_of(k) * 2 + jnp.where(k < depth, 1 - inner, inner)
        remote(
            row_block(d, other), row_block(d, other), row_pair_out_sem.at[d], row_pair_sem.at[d], twin
        ).wait_recv()
        block = pl.ds(pl.multiple_of(d * 2 * row_count, 2 * row_count), 2 * row_count)
        inputs = rows[block, 0:features]
        factors = rows[block, features : features + LANES].astype(jnp.float32)
        lane = lax.broadcasted_iota(jnp.int32, factors.shape, 1)
        chosen = (lane == expert) | (lane == expert + LANES // 2)
        factor = jnp.sum(jnp.where(chosen, factors, 0.0), axis=1, keepdims=True)
        gate = contract_rows(inputs, weights[0])
        up = contract_rows(inputs, weights[1])
        unit = lax.broadcasted_iota(jnp.int32, gate.shape, 1)
        scale = jnp.where(unit < hidden, factor, 1.0)
        units = (gate / (1.0 + jnp.exp(-gate)) * up * scale).astype(jnp.bfloat16)
        for c in range(4):
            span = pl.ds(c * width, width)
            parts[k, :, span] = jnp.dot(
                units, weights[2, :, span], preferred_element_type=jnp.float32
            ).astype(jnp.bfloat16)
        part_send(k).start()

        @pl.when((k > 0) & (k <= depth))
        def _():
            add_pair(k - 1)
            side_send(k - 1).start()

        @pl.when(k > depth)
        def _():
            add_both(k - 1)
            sum_send(k - 1).start()

    add_both(n - 1)
    for k in range(depth, n - 1):
        sum_send(k).wait_recv()

    @pl.loop(0, row_count // chunk)
    def _(i):
        at = pl.ds(pl.multiple_of(i * chunk, chunk), chunk)
        total = sums[n - 1, at, :].astype(jnp.float32)
        for k in range(depth - 1):
            total = total + sums_in[k, at, :].astype(jnp.float32)
        combined_ref[at, :] = total.astype(jnp.bfloat16)

    twin_piece.wait_send()
    shared_far.wait_send()
    shared_twin.wait_send()
    shared_relay.wait_send()
    row_relay(fs).wait_send()
    row_beside(fs).wait_send()

    @pl.when(outer < depth - 1)
    def _():
        row_onward(fs, 1).wait_send()

    @pl.when(outer > 0)
    def _():
        row_back().wait_send()

    def sent(place, step):
        source = place * 2 + inner

        @pl.when(onward_exists(step))
        def _():
            row_onward(source, step).wait_send()

        row_beside(source).wait_send()

    at_distance(sent)
    column_send(fs).wait_send()
    for k in range(1, n):
        piece_send(lax.rem(fs + k, n), 0).wait_send()
        piece_send(lax.rem(fs + k, n), 1).wait_send()
        column_send(lax.rem(fs + k, n)).wait_send()
        row_relay(lax.rem(fs + k, n)).wait_send()
    for k in range(n):
        part_send(k).wait_send()
    for k in range(depth):
        side_send(k).wait_send()
    for k in range(depth, n - 1):
        sum_send(k).wait_send()
    for copy in outs:
        copy.wait()


def direct_body(
    tokens,
    routes,
    route_weights,
    norm_gain,
    gate_trained,
    up_trained,
    down_trained,
    shared_gate_trained,
    shared_up_trained,
    shared_down_trained,
):
    gain_row = norm_gain[None, None, :]
    pieces = jnp.stack(
        [gate_trained * gain_row, up_trained * gain_row, down_trained], axis=1
    ).astype(jnp.bfloat16)
    shared_gain = norm_gain[None, :]
    shared_stack = jnp.stack(
        [shared_gate_trained * shared_gain, shared_up_trained * shared_gain, shared_down_trained],
        axis=0,
    ).astype(jnp.bfloat16)
    values = tokens.astype(jnp.float32)
    normed = (
        values * lax.rsqrt(jnp.mean(values * values, axis=1, keepdims=True) + epsilon)
    ).astype(jnp.bfloat16)
    n = lax.axis_size("fs")
    experts, _, hidden_piece, width = pieces.shape
    row_count, features = normed.shape
    shared_piece = shared_stack.shape[1]
    numbers = jnp.arange(LANES // 2, dtype=jnp.int32)
    factors = jnp.sum(
        jnp.where(routes[:, :, None] == numbers, route_weights[:, :, None], 0.0), axis=1
    )
    high = lax.reduce_precision(factors, 8, 7)
    rows = jnp.concatenate(
        [normed, high.astype(jnp.bfloat16), (factors - high).astype(jnp.bfloat16)], axis=1
    )
    hidden = n * hidden_piece
    hidden_all = hidden + shared_piece // 2
    vmem = pl.BlockSpec(memory_space=pltpu.VMEM)
    hbm = pl.BlockSpec(memory_space=pl.ANY)
    kind = jnp.bfloat16
    expert_shape = jax.ShapeDtypeStruct((1, hidden, features), kind)
    shared_shape = jax.ShapeDtypeStruct((shared_piece, features), kind)
    DMA = pltpu.SemaphoreType.DMA
    return pl.pallas_call(
        functools.partial(exchange_kernel, n),
        out_shape=(jax.ShapeDtypeStruct((row_count, features), kind),)
        + (expert_shape,) * 3
        + (shared_shape,) * 3,
        in_specs=[vmem] * 3,
        out_specs=(vmem,) + (hbm,) * 6,
        scratch_shapes=[
            pltpu.VMEM((3, hidden_all, features), kind),
            pltpu.VMEM((3, shared_piece, features), kind),
            pltpu.VMEM((experts * row_count, features + LANES), kind),
            pltpu.VMEM((n, 2 * row_count, features), kind),
            pltpu.VMEM((n, row_count, features), kind),
            pltpu.VMEM((n, row_count, features), kind),
            pltpu.VMEM((n // 2, row_count, features), kind),
            pltpu.VMEM((n // 2 - 1, row_count, features), kind),
            DMA((4,)),
            DMA((n, 2)),
            DMA((n, 2)),
            DMA((n,)),
            DMA((n,)),
            DMA((3,)),
            DMA((3,)),
            DMA((n,)),
            DMA((n // 2,)),
            DMA((1,)),
            DMA((n,)),
            DMA((n,)),
            DMA((n,)),
            DMA((n,)),
            DMA((n,)),
            DMA((n // 2,)),
            DMA((n // 2,)),
            DMA((n // 2 - 1,)),
            DMA((n // 2 - 1,)),
            DMA((6,)),
        ],
        compiler_params=pltpu.CompilerParams(
            collective_id=0, has_side_effects=True, vmem_limit_bytes=60 * 1024 * 1024
        ),
    )(pieces, shared_stack, rows)


def body(*arguments):
    experts = lax.axis_size("fs") * lax.axis_size("tp")
    per_token = arguments[1].shape[1]
    pairs = lax.axis_size("gr") == 2 and lax.axis_size("tp") == 2
    if pairs and lax.axis_size("fs") % 2 == 0 and experts <= min(2 * per_token, LANES // 2):
        return direct_body(*arguments)
    return dispatch_body(*arguments)


def solution(mesh):
    in_specs = (
        P(("gr", "fs", "tp"), None),
        P(("gr", "fs", "tp"), None),
        P(("gr", "fs", "tp"), None),
        P(("gr", "tp")),
        P(None, "fs", ("gr", "tp")),
        P(None, "fs", ("gr", "tp")),
        P(None, "fs", ("gr", "tp")),
        P("fs", ("gr", "tp")),
        P("fs", ("gr", "tp")),
        P("fs", ("gr", "tp")),
    )
    out_specs = (
        P(("gr", "fs", "tp"), None),
        P(("fs", "tp"), None, None),
        P(("fs", "tp"), None, None),
        P(("fs", "tp"), None, None),
        P("fs", None),
        P("fs", None),
        P("fs", None),
    )
    return jax.shard_map(body, mesh=mesh, in_specs=in_specs, out_specs=out_specs, check_vma=False)
```
